512 devices in a mesh: fs: 64 (over z, y), tp: 8 (over x, core).
Axes of the slice: x: 4, y: 4, z: 16, core: 2. Of those that a mesh axis runs over, the one named last changes fastest.
Arguments:
- tokens: bfloat16 [49152, 2048], P('fs'), may hold values from -6 to 6
- norm_gain: float32 [2048], replicated, may hold values from 0.1 to 1.9
- gate_weight: bfloat16 [2048, 5120], P('fs', 'tp'), may hold values from -0.125 to 0.125
- up_weight: bfloat16 [2048, 5120], P('fs', 'tp'), may hold values from -0.125 to 0.125
- down_weight: bfloat16 [5120, 2048], P('tp', 'fs'), may hold values from -0.078125 to 0.078125
Outputs:
- mixed: bfloat16 [49152, 2048], P(('fs', 'tp'))
The draws below stay inside these ranges and needn't reach their ends.
All inputs are finite; a program needn't handle non-finite values.
Results may differ from the reference program's by a relative error of at most 0.014.
Values may be sent and summed in bfloat16 or wider, within the bound.
A program may use at most 64 MiB of HBM per device.

```python
import jax
import jax.numpy as jnp
from jax import lax

D = 2048
FF = 5120
TOKENS = 49152
N_TP = 8


def levels(stream_key, dims, split, low, largest):
    level, own = 1.0, jax.random.fold_in(stream_key, 6)
    for dim, parts in split:
        steps = jnp.exp(jax.random.uniform(jax.random.fold_in(own, dim), (parts,), jnp.float32, low / len(split), largest / len(split)))
        level = level * jnp.repeat(steps, dims[dim] // parts).reshape([-1 if axis == dim else 1 for axis in range(len(dims))])
    return level


def noise(rng, shape, spread, bound, pieces=(), dtype=jnp.bfloat16):
    result = spread * jax.random.normal(rng, shape, jnp.float32)
    if pieces:
        result = result * levels(rng, shape, pieces, -0.22, 0.18)
    return jnp.clip(result, -bound, bound).astype(dtype)


def setup_inputs(seed: int = 0) -> dict:
    splits = jax.random.split(jax.random.key(seed), 6)
    tokens = noise(splits[0], (TOKENS, D), 1.0, 6.0, ((0, 64),))
    norm_gain = jnp.clip(1.0 + 0.18 * jax.random.normal(splits[1], (D,), jnp.float32), 0.1, 1.9)
    gate_weight = noise(splits[2], (D, FF), D ** -0.5, 0.125, ((0, 64), (1, 8)))
    up_weight = noise(splits[3], (D, FF), D ** -0.5, 0.125, ((0, 64), (1, 8)))
    down_weight = noise(splits[4], (FF, D), FF ** -0.5, 0.078125, ((0, 8), (1, 64)))
    return dict(tokens=tokens, norm_gain=norm_gain, gate_weight=gate_weight, up_weight=up_weight, down_weight=down_weight)


def reference(tokens, norm_gain, gate_weight, up_weight, down_weight):
    values = tokens.astype(jnp.float32)
    scale = lax.rsqrt(lax.optimization_barrier(jnp.mean(values * values, axis=-1, keepdims=True)) + 1e-06)
    normed = (values * scale * norm_gain).astype(jnp.bfloat16)
    gate_proj = jnp.dot(normed, gate_weight, preferred_element_type=jnp.float32)
    up_proj = jnp.dot(normed, up_weight, preferred_element_type=jnp.float32)
    hidden = (jax.nn.silu(gate_proj) * up_proj).astype(jnp.bfloat16)
    block = FF // N_TP
    total = jnp.zeros((tokens.shape[0], D), jnp.float32)
    for index in range(N_TP):
        part_sum = jnp.dot(hidden[:, index * block:(index + 1) * block], down_weight[index * block:(index + 1) * block, :], preferred_element_type=jnp.float32).astype(jnp.bfloat16)
        total = total + part_sum.astype(jnp.float32)
    return total.astype(jnp.bfloat16)
```

```python
import functools

import jax
import jax.numpy as jnp
from jax import lax
from jax.experimental import pallas as pl
from jax.experimental.pallas import tpu as pltpu
from jax.sharding import PartitionSpec as P

MESH = pl.DeviceIdType.MESH
NX, NY = 4, 4
PF = 256
LAG = 8
DIRS = (0, 1)
OFFSETS = (0, -1, 1, 2)


def kernel(nz, tok, gain, gate, up, down, out, tokv, gainv, nc, wq, wp, dq, dp, accq, accp, hid, own, dsend, drecv, xsend,
           xrecv, outb, ld, tokld, outs, d2s, d2r, xs, xr, *sems):
    fs, tp = lax.axis_index("fs"), lax.axis_index("tp")
    z, y = fs // NY, lax.rem(fs, NY)
    x, c = tp // 2, lax.rem(tp, 2)
    rows = tokv.shape[1]
    shard = gate.shape[0]
    half = shard // 2
    plane = shard * NY
    last = nz // 2
    part = NX * rows

    def zdev(d):
        return (lax.rem(z + d + nz, nz) * NY + y, tp)

    def ydev(d):
        return (z * NY + lax.rem(y + d + NY, NY), tp)

    def ypos(d):
        return lax.rem(y + d + NY, NY)

    def xdev(d):
        return (fs, lax.rem(x + d, NX) * 2 + c)

    partner = (fs, x * 2 + 1 - c)

    def remote(src, dst, ss, rs, dev):
        return pltpu.make_async_remote_copy(src_ref=src, dst_ref=dst, send_sem=ss, recv_sem=rs, device_id=dev,
                                            device_id_type=MESH)

    class Gather:
        def __init__(self, q, p, sems):
            self.q, self.p = q, p
            (self.qzs, self.qzr, self.qys, self.qyr, self.qws, self.qwr, self.pzs, self.pzr, self.pys, self.pyr, self.pws,
             self.pwr) = sems

        def at(self, ref, pair, side, yy, h=None):
            start = side * plane + yy * shard
            if h is None:
                return ref.at[pair, pl.ds(pl.multiple_of(start, half), shard), :]
            return ref.at[pair, pl.ds(pl.multiple_of(start + h * half, half), half), :]

        def q_send(self, s, d):
            pair, side = (0, 0) if isinstance(s, int) and s == 0 else (s, d)
            n = 2 * (s + 1) + d
            return remote(self.at(self.q, pair, side, y), self.at(self.q, s + 1, d, y), self.qzs.at[n], self.qzr.at[n],
                          zdev(1 - 2 * d))

        def q_send_last(self, d):
            return remote(self.at(self.q, last - 1, d, y, d), self.at(self.q, 0, 1, y, d), self.qzs.at[d], self.qzr.at[d],
                          zdev(1 - 2 * d))

        def y_send(self, ref, ss, rs, pair, side, n, d):
            here = self.at(ref, pair, side, y)
            return remote(here, here, ss.at[n, d], rs.at[n, d], ydev(1 - 2 * d))

        def y_recv(self, ref, ss, rs, pair, side, n, d):
            here = self.at(ref, pair, side, ypos(2 * d - 1))
            return remote(here, here, ss.at[n, d], rs.at[n, d], ydev(1 - 2 * d))

        def w_send(self, ref, ss, rs, pair, side, n, d):
            here = self.at(ref, pair, side, ypos(2 * d - 1), d)
            return remote(here, here, ss.at[n, d], rs.at[n, d], ydev(1 - 2 * d))

        def w_recv(self, ref, ss, rs, pair, side, n, d):
            here = self.at(ref, pair, side, ypos(2), d)
            return remote(here, here, ss.at[n, d], rs.at[n, d], ydev(1 - 2 * d))

        def q_y1(self, pair, side):
            for d in DIRS:
                self.y_send(self.q, self.qys, self.qyr, pair, side, 2 * pair + side, d).start()

        def q_y2(self, pair, side):
            for d in DIRS:
                self.y_recv(self.q, self.qys, self.qyr, pair, side, 2 * pair + side, d).wait_recv()
                self.w_send(self.q, self.qws, self.qwr, pair, side, 2 * pair + side, d).start()

        def q_y3(self, pair, side):
            for d in DIRS:
                self.w_recv(self.q, self.qws, self.qwr, pair, side, 2 * pair + side, d).wait_recv()

        def p_send(self, s, d, j):
            pair, side = (0, 0) if isinstance(s, int) and s == 0 else (s, d)
            yy = ypos(OFFSETS[j])
            n = 2 * (s + 1) + d
            return remote(self.at(self.p, pair, side, yy), self.at(self.p, s + 1, d, yy), self.pzs.at[n, j],
                          self.pzr.at[n, j], zdev(1 - 2 * d))

        def p_send_last(self, d, j):
            yy = ypos(OFFSETS[j])
            return remote(self.at(self.p, last - 1, d, yy), self.at(self.p, 0, 1, yy), self.pzs.at[1, j], self.pzr.at[1, j],
                          zdev(1 - 2 * d))

        def begin_q(self):
            for d in DIRS:
                self.q_send(0, d).start()
            self.q_y1(0, 0)

        def begin_p(self):
            for d in DIRS:
                self.y_send(self.p, self.pys, self.pyr, 0, 0, 0, d).start()
            for d in DIRS:
                self.p_send(0, d, 0).start()

        def begin_p2(self):
            for d in DIRS:
                self.y_recv(self.p, self.pys, self.pyr, 0, 0, 0, d).wait_recv()
                self.w_send(self.p, self.pws, self.pwr, 0, 0, 0, d).start()
                for e in DIRS:
                    self.p_send(0, e, 1 + d).start()

        def begin_p3(self):
            for d in DIRS:
                self.w_recv(self.p, self.pws, self.pwr, 0, 0, 0, d).wait_recv()
            for d in DIRS:
                self.p_send(0, d, 3).start()

        def step_q(self, s):
            @pl.when(s < last)
            def _():
                for d in DIRS:
                    self.q_send(s - 1, d).wait_recv()

                    @pl.when(s < last - 1)
                    def _():
                        self.q_send(s, d).start()

                    @pl.when(s == last - 1)
                    def _():
                        self.q_send_last(d).start()

                for d in DIRS:
                    self.q_y1(s, d)

            @pl.when(s == last)
            def _():
                for d in DIRS:
                    self.q_send_last(d).wait_recv()
                self.q_y1(0, 1)

        def step_p(self, s, j):
            @pl.when(s < last)
            def _():
                for d in DIRS:
                    self.p_send(s - 1, d, j).wait_recv()

                    @pl.when(s < last - 1)
                    def _():
                        self.p_send(s, d, j).start()

                    if d == j // 2:

                        @pl.when(s == last - 1)
                        def _():
                            self.p_send_last(d, j).start()

            @pl.when(s == last)
            def _():
                self.p_send_last(j // 2, j).wait_recv()

        def each_slot(self, s, act):
            @pl.when(s == 0)
            def _():
                act(0, 0)

            @pl.when(jnp.logical_and(s > 0, s < last))
            def _():
                act(s, 0)
                act(s, 1)

            @pl.when(s == last)
            def _():
                act(0, 1)

        def finish(self):
            def one(n, _):
                for d in DIRS:
                    self.y_send(self.q, self.qys, self.qyr, n // 2, lax.rem(n, 2), n, d).wait_send()
                    self.w_send(self.q, self.qws, self.qwr, n // 2, lax.rem(n, 2), n, d).wait_send()

                return 0

            lax.fori_loop(0, nz, one, 0)
            for d in DIRS:
                self.q_send_last(d).wait_send()
                self.y_send(self.p, self.pys, self.pyr, 0, 0, 0, d).wait_send()
                self.w_send(self.p, self.pws, self.pwr, 0, 0, 0, d).wait_send()
            for j in range(NY):
                self.p_send_last(j // 2, j).wait_send()

            def two(s, _):
                for d in DIRS:
                    self.q_send(s, d).wait_send()
                    for j in range(NY):
                        self.p_send(s, d, j).wait_send()
                return 0

            lax.fori_loop(0, last - 1, two, 0)

    first = Gather(wq, wp, sems[:12])
    second = Gather(dq, dp, sems[12:])

    unit = gate.shape[1]
    mine = pl.ds(pl.multiple_of(y * shard, shard), shard)
    qf = unit - PF
    loads = [
        (gate.at[:, pl.ds(PF, qf)], wq.at[0, mine, pl.ds(0, qf)]),
        (up.at[:, pl.ds(PF, qf)], wq.at[0, mine, pl.ds(qf, qf)]),
        (gate.at[:, pl.ds(0, PF)], wp.at[0, mine, pl.ds(0, PF)]),
        (up.at[:, pl.ds(0, PF)], wp.at[0, mine, pl.ds(PF, PF)]),
        (down.at[:, pl.ds(PF, qf)], dq.at[0, mine, :]),
        (down.at[:, pl.ds(0, PF)], dp.at[0, mine, :]),
        (gain, gainv),
    ]
    loads = [pltpu.make_async_copy(a, b, ld.at[i]) for i, (a, b) in enumerate(loads)]
    for copy in loads:
        copy.start()
    barrier = pltpu.get_barrier_semaphore()
    peers = [zdev(1), zdev(-1), ydev(1), ydev(-1), partner] + [xdev(d) for d in range(1, NX)]
    for dev in peers:
        pl.semaphore_signal(barrier, inc=1, device_id=dev, device_id_type=MESH)
    tok_loads = []
    for i in range(2 * NX):
        core = c if i < NX else 1 - c
        owner = lax.rem(x + i % NX, NX) * 2 + core
        tok_loads.append(pltpu.make_async_copy(tok.at[pl.ds(pl.multiple_of(owner * rows, 32), rows), :], tokv.at[i], tokld.at[i]))
        tok_loads[-1].start()
    pl.semaphore_wait(barrier, len(peers))

    loads[0].wait()
    loads[1].wait()
    first.begin_q()
    loads[2].wait()
    loads[3].wait()
    first.begin_p()
    for copy in loads[4:]:
        copy.wait()
    for copy in tok_loads:
        copy.wait()
    first.begin_p2()

    sub = 32

    def norm(i):
        def some(r, _):
            at = pl.ds(pl.multiple_of(r * sub, sub), sub)
            to = pl.ds(pl.multiple_of(i * rows + r * sub, sub), sub)
            values = tokv[i, at, :].astype(jnp.float32)
            scale = lax.rsqrt(jnp.mean(values * values, axis=-1, keepdims=True) + 1e-6)
            normed = (values * scale * gainv[...]).astype(jnp.bfloat16)
            for k in range(nz):
                nc[k, to, :] = normed[:, k * plane:(k + 1) * plane]
            return 0

        lax.fori_loop(0, rows // sub, some, 0)
        at = pl.ds(pl.multiple_of(i * rows, sub), rows)
        accq[at, :] = jnp.zeros((rows, 2 * qf), jnp.float32)
        accp[at, :] = jnp.zeros((rows, 2 * PF), jnp.float32)

    block = part // 2

    def project(s, j):
        at = pl.ds(j * block, block)
        za = lax.rem(z - lax.rem(s, last) + nz, nz)
        zb = lax.rem(z + s, nz)
        left = jnp.concatenate([nc[za, at, :], nc[zb, at, :]], axis=1)
        pair = lax.rem(s, last)
        accq[at, :] += jnp.dot(left, wq[pair], preferred_element_type=jnp.float32)
        accp[at, :] += jnp.dot(left, wp[pair], preferred_element_type=jnp.float32)

    def gated(j):
        at = pl.ds(j * block, block)
        g, u = accp[at, :PF], accp[at, PF:]
        hid[at, :PF] = (g / (1.0 + jnp.exp(-g)) * u).astype(jnp.bfloat16)
        g, u = accq[at, :qf], accq[at, qf:]
        hid[at, PF:] = (g / (1.0 + jnp.exp(-g)) * u).astype(jnp.bfloat16)

    def dot_t(a, b):
        return lax.dot_general(a, b, (((1,), (1,)), ((), ())), preferred_element_type=jnp.float32)

    def to_partner(pair):
        return remote(dsend.at[pair], drecv.at[pair], d2s.at[pair], d2r.at[pair], partner)

    def to_owner(pair, d):
        return remote(xsend.at[pair, d - 1], xrecv.at[pair, d - 1], xs.at[pair, d - 1], xr.at[pair, d - 1], xdev(d))

    def to_out(s, side):
        pair = lax.rem(s, last)
        zz = lax.rem(z + s, nz) if side else lax.rem(z - pair + nz, nz)
        return pltpu.make_async_copy(outb.at[pair, :, pl.ds(side * plane, plane)],
                                     out.at[:, pl.ds(pl.multiple_of(zz * plane, plane), plane)], outs.at[pair, side])

    def mix(s):
        pair = lax.rem(s, last)
        for j in (2, 3, 0, 1):
            at = pl.ds(j * block, block)
            here = dot_t(hid[at, :PF], dp[pair]) + dot_t(hid[at, PF:], dq[pair])
            if j >= 2:
                dsend[pair, pl.ds((j - 2) * block, block), :] = here.astype(jnp.bfloat16)
                if j == 3:
                    to_partner(pair).start()
            else:
                own[pair, at, :] = here

    def chip_sum(s):
        pair = lax.rem(s, last)
        to_partner(pair).wait_recv()
        for d in (2, 1, 3, 0):
            at = pl.ds(d * rows, rows)
            both = own[pair, at, :] + drecv[pair, at, :].astype(jnp.float32)
            if d:
                xsend[pair, d - 1] = both.astype(jnp.bfloat16)
            else:
                own[pair, at, :] = both
        for d in (2, 1, 3):
            to_owner(pair, d).start()

    def total(s):
        pair = lax.rem(s, last)
        both = own[pair, pl.ds(0, rows), :]
        for d in range(1, NX):
            to_owner(pair, d).wait_recv()
            both += xrecv[pair, d - 1].astype(jnp.float32)
        outb[pair] = both.astype(jnp.bfloat16)
        for side in DIRS:
            to_out(s, side).start()

    def compute(t, j):
        if j == 0:
            first.each_slot(t - 2, first.q_y3)

        @pl.when(t <= 2)
        def _():
            norm((t - 1) * 4 + j)

        @pl.when(jnp.logical_and(t >= 3, t <= last + 2))
        def _():
            project(t - 2, j)

        @pl.when(t == last + 2)
        def _():
            gated(j)

    def inside(v):
        return jnp.logical_and(v >= 1, v <= last)

    def body(t, _):
        d = t - LAG

        @pl.when(t <= last)
        def _():
            first.step_q(t)

        for j in range(NY):
            @pl.when(t <= last)
            def _():
                first.step_p(t, j)

            if j == 0:
                @pl.when(t == 1)
                def _():
                    first.begin_p3()

                first.each_slot(t - 1, first.q_y2)

            @pl.when(t <= last + 2)
            def _():
                compute(t, j)

        @pl.when(d == 0)
        def _():
            second.begin_q()
            second.begin_p()

        @pl.when(inside(d))
        def _():
            second.step_q(d)

        @pl.when(d == 1)
        def _():
            second.begin_p2()
            second.begin_p3()

        second.each_slot(d - 1, second.q_y2)

        u = t - last - 2

        @pl.when(inside(u - 1))
        def _():
            chip_sum(u - 1)

        for j in range(2):
            @pl.when(inside(d))
            def _():
                second.step_p(d, j)

        @pl.when(inside(u))
        def _():
            @pl.when(u == 1)
            def _():
                second.each_slot(0, second.q_y3)

            second.each_slot(u, second.q_y3)
            mix(u)

        for j in range(2, 4):
            @pl.when(inside(d))
            def _():
                second.step_p(d, j)

        @pl.when(inside(u - 3))
        def _():
            total(u - 3)

        return 0

    lax.fori_loop(1, 2 * last + 6, body, 0)

    first.finish()
    second.finish()

    def done(s, _):
        pair = lax.rem(s, last)
        to_partner(pair).wait_send()
        for d in range(1, NX):
            to_owner(pair, d).wait_send()
        for side in DIRS:
            to_out(s, side).wait()
        return 0

    lax.fori_loop(1, last + 1, done, 0)


def solution(mesh):
    nz = mesh.shape["fs"] // NY

    def per_device(tokens, norm_gain, gate, up, down):
        m, width = tokens.shape
        shard, unit = gate.shape
        rows = m // (2 * NX)
        part = NX * rows
        qf = unit - PF
        pairs = nz // 2
        deep = 2 * NY * shard
        bf, f32, dma = jnp.bfloat16, jnp.float32, pltpu.SemaphoreType.DMA
        gather_sems = [dma((nz,)), dma((nz,))] + [dma((nz, 2))] * 4 + [dma((nz, NY))] * 2 + [dma((1, 2))] * 4
        return pl.pallas_call(
            functools.partial(kernel, nz),
            out_shape=jax.ShapeDtypeStruct((rows, width), bf),
            in_specs=[pl.BlockSpec(memory_space=pltpu.HBM)] * 5,
            out_specs=pl.BlockSpec(memory_space=pltpu.HBM),
            scratch_shapes=[
                pltpu.VMEM((2 * NX, rows, width), bf),
                pltpu.VMEM((1, width), f32),
                pltpu.VMEM((nz, m, NY * shard), bf),
                pltpu.VMEM((pairs, deep, 2 * qf), bf),
                pltpu.VMEM((pairs, deep, 2 * PF), bf),
                pltpu.VMEM((pairs, deep, qf), bf),
                pltpu.VMEM((pairs, deep, PF), bf),
                pltpu.VMEM((m, 2 * qf), f32),
                pltpu.VMEM((m, 2 * PF), f32),
                pltpu.VMEM((m, unit), bf),
                pltpu.VMEM((pairs, part, deep), f32),
                pltpu.VMEM((pairs, part, deep), bf),
                pltpu.VMEM((pairs, part, deep), bf),
                pltpu.VMEM((pairs, NX - 1, rows, deep), bf),
                pltpu.VMEM((pairs, NX - 1, rows, deep), bf),
                pltpu.VMEM((pairs, rows, deep), bf),
                dma((7,)),
                dma((2 * NX,)),
                dma((pairs, 2)),
                dma((pairs,)),
                dma((pairs,)),
                dma((pairs, NX - 1)),
                dma((pairs, NX - 1)),
            ]
            + gather_sems * 2,
            compiler_params=pltpu.CompilerParams(collective_id=0, has_side_effects=True, vmem_limit_bytes=60 * 1024 * 1024),
        )(tokens, norm_gain.reshape(1, width), gate, up, down.T)

    return jax.shard_map(
        per_device,
        mesh=mesh,
        in_specs=(P("fs", None), P(), P("fs", "tp"), P("fs", "tp"), P("tp", "fs")),
        out_specs=P(("fs", "tp"), None),
        check_vma=False,
    )
```

```python
import functools

import jax
import jax.numpy as jnp
from jax import lax
from jax.experimental import pallas as pl
from jax.experimental.pallas import tpu as pltpu
from jax.sharding import PartitionSpec as P

MESH = pl.DeviceIdType.MESH
NX, NY = 4, 4
PF = 256
LAG = 8
MIX = 3
DIRS = (0, 1)
OFFSETS = (0, -1, 1, 2)
RING = 4


def kernel(nz, tok, gain, gate, up, down, out, tokv, gainv, nc, wq, wp, dq, dp, accq, accp, hid, own, dsend, drecv, xsend,
           xrecv, outb, ld, outs, d2s, d2r, xs, xr, *sems):
    fs, tp = lax.axis_index("fs"), lax.axis_index("tp")
    z, y = fs // NY, lax.rem(fs, NY)
    x, c = tp // 2, lax.rem(tp, 2)
    rows = tokv.shape[1]
    shard = gate.shape[0]
    half = shard // 2
    plane = shard * NY
    last = nz // 2
    part = NX * rows
    scope = jax.named_scope

    def zdev(d):
        return (lax.rem(z + d + nz, nz) * NY + y, tp)

    def ydev(d):
        return (z * NY + lax.rem(y + d + NY, NY), tp)

    def ypos(d):
        return lax.rem(y + d + NY, NY)

    def xdev(d):
        return (fs, lax.rem(x + d, NX) * 2 + c)

    partner = (fs, x * 2 + 1 - c)

    def remote(src, dst, ss, rs, dev):
        return pltpu.make_async_remote_copy(src_ref=src, dst_ref=dst, send_sem=ss, recv_sem=rs, device_id=dev,
                                            device_id_type=MESH)

    class Gather:
        def __init__(self, q, p, sems):
            self.q, self.p = q, p
            (self.qzs, self.qzr, self.qls, self.qlr, self.pzs, self.pzr, self.pls, self.plr, self.yes, self.yer, self.yds,
             self.ydr) = sems

        def at(self, ref, pair, side, yy, h=None):
            start, size = yy * shard + (0 if h is None else h * half), shard if h is None else half
            if side is None:
                return ref.at[pair, :, pl.ds(pl.multiple_of(start, half), size), :]
            return ref.at[pair, side, pl.ds(pl.multiple_of(start, half), size), :]

        def q_send(self, s, d):
            pair, side = (0, 0) if isinstance(s, int) and s == 0 else (s, d)
            n = lax.rem(s + 1, RING)
            return remote(self.at(self.q, pair, side, y), self.at(self.q, s + 1, d, y), self.qzs.at[d], self.qzr.at[n, d],
                          zdev(1 - 2 * d))

        def q_last(self, d):
            return remote(self.at(self.q, last - 1, d, y, d), self.at(self.q, 0, 1, y, d), self.qls.at[d], self.qlr.at[d],
                          zdev(1 - 2 * d))

        def where(self, kind):
            if isinstance(kind, int):
                ref, pair, side = ((self.q, 0, 0), (self.q, 0, 1), (self.p, 0, 0))[kind]
                return ref, pair, side, self.yes, self.yer, kind
            return self.q, kind, None, self.yds, self.ydr, kind

        def y_sem(self, kind, ss, rs, hop, d):
            if isinstance(kind, int):
                return ss.at[kind, hop, d], rs.at[kind, hop, d]
            return ss.at[hop, d], rs.at[kind - 1, hop, d]

        def y_send(self, kind, d):
            ref, pair, side, ss, rs, n = self.where(kind)
            here = self.at(ref, pair, side, y)
            return remote(here, here, *self.y_sem(kind, ss, rs, 0, d), ydev(1 - 2 * d))

        def y_recv(self, kind, d):
            ref, pair, side, ss, rs, n = self.where(kind)
            here = self.at(ref, pair, side, ypos(2 * d - 1))
            return remote(here, here, *self.y_sem(kind, ss, rs, 0, d), ydev(1 - 2 * d))

        def w_send(self, kind, d):
            ref, pair, side, ss, rs, n = self.where(kind)
            here = self.at(ref, pair, side, ypos(2 * d - 1), d)
            return remote(here, here, *self.y_sem(kind, ss, rs, 1, d), ydev(1 - 2 * d))

        def w_recv(self, kind, d):
            ref, pair, side, ss, rs, n = self.where(kind)
            here = self.at(ref, pair, side, ypos(2), d)
            return remote(here, here, *self.y_sem(kind, ss, rs, 1, d), ydev(1 - 2 * d))

        def y1(self, kind):
            for d in DIRS:
                if not isinstance(kind, int):

                    @pl.when(kind > 1)
                    def _():
                        self.y_send(kind - 1, d).wait_send()

                self.y_send(kind, d).start()

        def y2(self, kind):
            for d in DIRS:
                self.y_recv(kind, d).wait_recv()
                if not isinstance(kind, int):

                    @pl.when(kind > 1)
                    def _():
                        self.w_send(kind - 1, d).wait_send()

                self.w_send(kind, d).start()

        def y3(self, kind):
            for d in DIRS:
                self.w_recv(kind, d).wait_recv()

        def at_step(self, s, act):
            @pl.when(s == 0)
            def _():
                act(0)

            @pl.when(jnp.logical_and(s > 0, s < last))
            def _():
                act(s)

            @pl.when(s == last)
            def _():
                act(1)

        def p_send(self, s, d, j):
            pair, side = (0, 0) if isinstance(s, int) and s == 0 else (s, d)
            yy = ypos(OFFSETS[j])
            n = lax.rem(s + 1, RING)
            return remote(self.at(self.p, pair, side, yy), self.at(self.p, s + 1, d, yy), self.pzs.at[d, j],
                          self.pzr.at[n, d, j], zdev(1 - 2 * d))

        def p_last(self, d, j):
            yy = ypos(OFFSETS[j])
            return remote(self.at(self.p, last - 1, d, yy), self.at(self.p, 0, 1, yy), self.pls.at[j], self.plr.at[j],
                          zdev(1 - 2 * d))

        def begin_q(self):
            for d in DIRS:
                self.q_send(0, d).start()

        def begin_p(self, j):
            for d in DIRS:
                self.p_send(0, d, j).start()

        def step_q(self, s):
            @pl.when(s < last)
            def _():
                for d in DIRS:
                    self.q_send(s - 1, d).wait_recv()

                    @pl.when(s < last - 1)
                    def _():
                        self.q_send(s - 1, d).wait_send()
                        self.q_send(s, d).start()

                    @pl.when(s == last - 1)
                    def _():
                        self.q_last(d).start()

                self.y1(s)

            @pl.when(s == last)
            def _():
                for d in DIRS:
                    self.q_last(d).wait_recv()
                self.y1(1)

        def step_p(self, s, j):
            @pl.when(s < last)
            def _():
                for d in DIRS:
                    self.p_send(s - 1, d, j).wait_recv()

                    @pl.when(s < last - 1)
                    def _():
                        self.p_send(s - 1, d, j).wait_send()
                        self.p_send(s, d, j).start()

                    if d == j // 2:

                        @pl.when(s == last - 1)
                        def _():
                            self.p_last(d, j).start()

            @pl.when(s == last)
            def _():
                self.p_last(j // 2, j).wait_recv()

        def finish(self):
            for d in DIRS:
                self.q_send(last - 2, d).wait_send()
                self.q_last(d).wait_send()
                for kind in (0, 1, 2, jnp.int32(last - 1)):
                    self.y_send(kind, d).wait_send()
                    self.w_send(kind, d).wait_send()
                for j in range(NY):
                    self.p_send(last - 2, d, j).wait_send()
            for j in range(NY):
                self.p_last(j // 2, j).wait_send()

    first = Gather(wq, wp, sems[:12])
    second = Gather(dq, dp, sems[12:])

    unit = gate.shape[1]
    mine = pl.ds(pl.multiple_of(y * shard, shard), shard)
    qf = unit - PF
    loads = [
        (gate.at[:, pl.ds(0, PF)], wp.at[0, 0, mine, pl.ds(0, PF)]),
        (up.at[:, pl.ds(0, PF)], wp.at[0, 0, mine, pl.ds(PF, PF)]),
        (gate.at[:, pl.ds(PF, qf)], wq.at[0, 0, mine, pl.ds(0, qf)]),
        (up.at[:, pl.ds(PF, qf)], wq.at[0, 0, mine, pl.ds(qf, qf)]),
        (down.at[:, pl.ds(PF, qf)], dq.at[0, 0, mine, :]),
        (down.at[:, pl.ds(0, PF)], dp.at[0, 0, mine, :]),
        (gain, gainv),
    ]
    loads = [pltpu.make_async_copy(a, b, ld.at[i]) for i, (a, b) in enumerate(loads)]
    for copy in loads:
        copy.start()
    barrier = pltpu.get_barrier_semaphore()
    peers = [zdev(1), zdev(-1), ydev(1), ydev(-1), partner] + [xdev(d) for d in range(1, NX)]
    for dev in peers:
        pl.semaphore_signal(barrier, inc=1, device_id=dev, device_id_type=MESH)
    tok_sem = ld.at[len(loads)]
    for i in range(2 * NX):
        core = c if i < NX else 1 - c
        owner = lax.rem(x + i % NX, NX) * 2 + core
        pltpu.make_async_copy(tok.at[pl.ds(pl.multiple_of(owner * rows, 32), rows), :], tokv.at[i], tok_sem).start()
    sub = 32

    def norm(i):
        def some(r, _):
            at = pl.ds(pl.multiple_of(r * sub, sub), sub)
            to = pl.ds(pl.multiple_of(i * rows + r * sub, sub), sub)
            values = tokv[i, at, :].astype(jnp.float32)
            scale = lax.rsqrt(jnp.mean(values * values, axis=-1, keepdims=True) + 1e-6)
            normed = (values * scale * gainv[...]).astype(jnp.bfloat16)
            for k in range(nz):
                nc[k, to, :] = normed[:, k * plane:(k + 1) * plane]
            return 0

        lax.fori_loop(0, rows // sub, some, 0)
        at = pl.ds(pl.multiple_of(i * rows, sub), rows)
        accq[at, :] = jnp.zeros((rows, 2 * qf), jnp.float32)
        accp[at, :] = jnp.zeros((rows, 2 * PF), jnp.float32)

    EARLY = 2

    with scope("barrier"):
        pl.semaphore_wait(barrier, len(peers))
    with scope("b1"):
        loads[0].wait()
        loads[1].wait()
        first.y1(2)
        first.begin_p(0)
        loads[2].wait()
        loads[3].wait()
        first.begin_q()
    with scope("b2"):
        for copy in loads[4:]:
            copy.wait()
        pltpu.make_async_copy(tokv, tokv, tok_sem).wait()
        for i in range(EARLY):
            norm(i)
    with scope("b3"):
        first.y2(2)
        first.begin_p(1)
        first.begin_p(2)
        first.y1(0)

    block = part // 2

    def project(s, j):
        at = pl.ds(j * block, block)
        pair = lax.rem(s, last)
        za, zb = lax.rem(z - pair + nz, nz), lax.rem(z + s, nz)
        left = jnp.concatenate([nc[za, at, :], nc[zb, at, :]], axis=1)
        accq[at, :] += jnp.dot(left, wq[pair].reshape(2 * plane, 2 * qf), preferred_element_type=jnp.float32)
        accp[at, :] += jnp.dot(left, wp[pair].reshape(2 * plane, 2 * PF), preferred_element_type=jnp.float32)

    def gated(j):
        at = pl.ds(j * block, block)
        g, u = accp[at, :PF], accp[at, PF:]
        hid[at, :PF] = (g / (1.0 + jnp.exp(-g)) * u).astype(jnp.bfloat16)
        g, u = accq[at, :qf], accq[at, qf:]
        hid[at, PF:] = (g / (1.0 + jnp.exp(-g)) * u).astype(jnp.bfloat16)

    def dot_t(a, b):
        return lax.dot_general(a, b, (((1,), (1,)), ((), ())), preferred_element_type=jnp.float32)

    class Columns:
        def __init__(self, s, side):
            self.s = s
            self.pair = 0 if side is not None else s
            self.sides = DIRS if side is None else (side,)
            self.cols = pl.ds(self.sides[0] * plane, plane * len(self.sides))

        def to_partner(self):
            return remote(dsend.at[self.pair, :, self.cols], drecv.at[self.pair, :, self.cols], d2s.at[self.s], d2r.at[self.s],
                          partner)

        def to_owner(self, d):
            return remote(xsend.at[self.pair, d - 1, :, self.cols], xrecv.at[self.pair, d - 1, :, self.cols],
                          xs.at[self.s, d - 1], xr.at[self.s, d - 1], xdev(d))

        def to_out(self, side):
            zz = lax.rem(z + self.s, nz) if side else lax.rem(z - self.pair + nz, nz)
            return pltpu.make_async_copy(outb.at[self.pair, :, pl.ds(side * plane, plane)],
                                         out.at[:, pl.ds(pl.multiple_of(zz * plane, plane), plane)],
                                         outs.at[self.pair, side])

        def mix(self, blocks):
            n = len(self.sides)
            if n == 2:
                bp, bq = dp[self.pair].reshape(2 * plane, PF), dq[self.pair].reshape(2 * plane, qf)
            else:
                bp, bq = dp[0, self.sides[0]], dq[0, self.sides[0]]
            for j in blocks:
                at = pl.ds(j * block, block)
                here = dot_t(hid[at, :PF], bp) + dot_t(hid[at, PF:], bq)
                if j >= 2:
                    dsend[self.pair, pl.ds((j - 2) * block, block), self.cols] = here.astype(jnp.bfloat16)
                else:
                    own[self.pair, at, self.cols] = here

        def chip_sum(self):
            self.to_partner().wait_recv()
            for d in (2, 1, 3, 0):
                at = pl.ds(d * rows, rows)
                both = own[self.pair, at, self.cols] + drecv[self.pair, at, self.cols].astype(jnp.float32)
                if d:
                    xsend[self.pair, d - 1, :, self.cols] = both.astype(jnp.bfloat16)
                else:
                    own[self.pair, at, self.cols] = both
            for d in (2, 1, 3):
                self.to_owner(d).start()

        def total(self):
            both = own[self.pair, pl.ds(0, rows), self.cols]
            for d in range(1, NX):
                self.to_owner(d).wait_recv()
                both += xrecv[self.pair, d - 1, :, self.cols].astype(jnp.float32)
            outb[self.pair, :, self.cols] = both.astype(jnp.bfloat16)
            for side in self.sides:
                self.to_out(side).start()

        def finish(self):
            self.to_partner().wait_send()
            for d in range(1, NX):
                self.to_owner(d).wait_send()
            for side in self.sides:
                self.to_out(side).wait()

    def columns(s, act):
        @pl.when(s == 0)
        def _():
            act(Columns(0, 0))

        @pl.when(jnp.logical_and(s > 0, s < last))
        def _():
            act(Columns(s, None))

        @pl.when(s == last)
        def _():
            act(Columns(last, 1))

    def compute(t, j):
        @pl.when(t <= 2)
        def _():
            i = EARLY + (t - 1) * 4 + j

            @pl.when(i < 2 * NX)
            def _():
                norm(i)

        @pl.when(jnp.logical_and(t >= 3, t <= last + 2))
        def _():
            project(t - 2, j)

        @pl.when(t == last + 2)
        def _():
            gated(j)

    def inside(v):
        return jnp.logical_and(v >= 1, v <= last)

    def both(a, b):
        return jnp.logical_and(a, b)

    def body(t, _):
        d = t - LAG
        u = d - MIX

        def when(cond, name, act):
            @pl.when(cond)
            def _():
                with scope(name):
                    act()

        when(t <= last, "q", lambda: first.step_q(t))
        when(t <= last, "p0", lambda: first.step_p(t, 0))

        @pl.when(t == 1)
        def _():
            with scope("y3p"):
                first.y3(2)
                first.begin_p(3)

        when(t <= last, "p1", lambda: first.step_p(t, 1))
        when(t <= last + 1, "y2", lambda: first.at_step(t - 1, first.y2))
        when(t <= last + 2, "y3", lambda: first.at_step(t - 2, first.y3))
        when(t <= last + 2, "c0", lambda: compute(t, 0))
        when(t <= last + 2, "c1", lambda: compute(t, 1))
        when(t <= last, "p2", lambda: first.step_p(t, 2))
        when(t <= last + 2, "c2", lambda: compute(t, 2))
        when(t <= last, "p3", lambda: first.step_p(t, 3))
        when(t <= last + 2, "c3", lambda: compute(t, 3))

        when(t == 2, "e1", lambda: (second.y1(2), second.y1(0)))
        when(t == 4, "e2", lambda: (second.y2(2), second.y2(0)))
        when(t == 6, "e3", lambda: (second.y3(2), second.y3(0)))

        @pl.when(d == 0)
        def _():
            second.begin_q()
            for j in range(NY):
                second.begin_p(j)

        when(inside(d), "dq", lambda: second.step_q(d))
        when(both(u >= 1, u <= last + 1), "chip", lambda: columns(u - 1, Columns.chip_sum))
        when(inside(d), "dp0", lambda: second.step_p(d, 0))
        when(both(u >= 1, u <= last), "dy3", lambda: second.at_step(u, second.y3))

        @pl.when(both(u >= 0, u <= last))
        def _():
            with scope("mixa"):
                columns(u, lambda k: (k.mix((2, 3)), k.to_partner().start()))

        when(inside(d), "dp1", lambda: second.step_p(d, 1))

        @pl.when(both(u >= 0, u <= last))
        def _():
            with scope("mixb"):
                columns(u, lambda k: k.mix((0, 1)))

        when(inside(d), "dp2", lambda: second.step_p(d, 2))
        when(inside(d), "dp3", lambda: second.step_p(d, 3))
        when(inside(d - 1), "dy2", lambda: second.at_step(d - 1, second.y2))
        when(both(u >= 3, u <= last + 3), "total", lambda: columns(u - 3, Columns.total))
        return 0

    lax.fori_loop(1, last + LAG + MIX + 4, body, 0)

    with scope("finish"):
        first.finish()
        second.finish()

        def done(s, _):
            columns(s, Columns.finish)
            return 0

        lax.fori_loop(0, last + 1, done, 0)


def solution(mesh):
    nz = mesh.shape["fs"] // NY

    def per_device(tokens, norm_gain, gate, up, down):
        m, width = tokens.shape
        shard, unit = gate.shape
        rows = m // (2 * NX)
        part = NX * rows
        qf = unit - PF
        pairs = nz // 2
        plane = NY * shard
        deep = 2 * plane
        bf, f32, dma = jnp.bfloat16, jnp.float32, pltpu.SemaphoreType.DMA
        gather_sems = [
            dma((2,)), dma((RING, 2)), dma((2,)), dma((2,)),
            dma((2, NY)), dma((RING, 2, NY)), dma((NY,)), dma((NY,)),
            dma((3, 2, 2)), dma((3, 2, 2)), dma((2, 2)), dma((pairs - 1, 2, 2)),
        ]
        return pl.pallas_call(
            functools.partial(kernel, nz),
            out_shape=jax.ShapeDtypeStruct((rows, width), bf),
            in_specs=[pl.BlockSpec(memory_space=pltpu.HBM)] * 5,
            out_specs=pl.BlockSpec(memory_space=pltpu.HBM),
            scratch_shapes=[
                pltpu.VMEM((2 * NX, rows, width), bf),
                pltpu.VMEM((1, width), f32),
                pltpu.VMEM((nz, m, plane), bf),
                pltpu.VMEM((pairs, 2, plane, 2 * qf), bf),
                pltpu.VMEM((pairs, 2, plane, 2 * PF), bf),
                pltpu.VMEM((pairs, 2, plane, qf), bf),
                pltpu.VMEM((pairs, 2, plane, PF), bf),
                pltpu.VMEM((m, 2 * qf), f32),
                pltpu.VMEM((m, 2 * PF), f32),
                pltpu.VMEM((m, unit), bf),
                pltpu.VMEM((pairs, part, deep), f32),
                pltpu.VMEM((pairs, part, deep), bf),
                pltpu.VMEM((pairs, part, deep), bf),
                pltpu.VMEM((pairs, NX - 1, rows, deep), bf),
                pltpu.VMEM((pairs, NX - 1, rows, deep), bf),
                pltpu.VMEM((pairs, rows, deep), bf),
                dma((8,)),
                dma((pairs, 2)),
                dma((pairs + 1,)),
                dma((pairs + 1,)),
                dma((pairs + 1, NX - 1)),
                dma((pairs + 1, NX - 1)),
            ]
            + gather_sems * 2,
            compiler_params=pltpu.CompilerParams(collective_id=0, has_side_effects=True, vmem_limit_bytes=60 * 1024 * 1024),
        )(tokens, norm_gain.reshape(1, width), gate, up, down.T)

    return jax.shard_map(
        per_device,
        mesh=mesh,
        in_specs=(P("fs", None), P(), P("fs", "tp"), P("fs", "tp"), P("tp", "fs")),
        out_specs=P(("fs", "tp"), None),
        check_vma=False,
    )
```
